512 devices in a mesh: ep: 16 (over y, x), tp: 32 (over z, core).
Axes of the slice: x: 4, y: 4, z: 16, core: 2. Of those that a mesh axis runs over, the one named last changes fastest.
Arguments:
- tokens: bfloat16 [3584, 4096], P('ep', 'tp'), may hold values from -6 to 6
- picks: int32 [16, 16, 56], P('ep'), may hold values from 0 to 223, as said below
- pick_weights: float32 [16, 16, 56], P('ep'), may hold values from 0.1 to 1
- gate_weight: bfloat16 [16, 1280, 4096], P('ep', 'tp'), may hold values from -0.09375 to 0.09375
- up_weight: bfloat16 [16, 1280, 4096], P('ep', 'tp'), may hold values from -0.09375 to 0.09375
- down_weight: bfloat16 [16, 1280, 4096], P('ep', None, 'tp'), may hold values from -0.15625 to 0.15625
- dense_gate: bfloat16 [5120, 4096], P('tp'), may hold values from -0.09375 to 0.09375
- dense_up: bfloat16 [5120, 4096], P('tp'), may hold values from -0.09375 to 0.09375
- dense_down: bfloat16 [5120, 4096], P('tp'), may hold values from -0.078125 to 0.078125
- branch_gate: float32 [4096], P('tp'), may hold values from -6 to 6
Outputs:
- mixed: bfloat16 [3584, 4096], P('ep', 'tp')
The draws below stay inside these ranges and needn't reach their ends.
Inputs may be any that keep to these rules, and one draw needn't show every extreme that they name: For each block s and expert e, the 56 entries picks[s, e, :] are distinct rows of that block.
All inputs are finite; a program needn't handle non-finite values.
Results may differ from the reference program's by a relative error of at most 0.014.
Values may be sent and summed in bfloat16 or wider, within the bound.
No kernel may reach another device: no remote copies, remote signals or barrier semaphores. Data moves between devices by JAX's collectives and lax.ppermute only.
A program may use at most 64 MiB of HBM per device.

```python
import jax
import jax.numpy as jnp

D = 4096
FF = 1280
DF = 5120
TOK_DEV = 224
SLOTS = 56
EXPERTS = 16
TOKENS = 3584
N_EP = 16
N_TP = 32


def draw_picks(key, part):
    key_list = jax.random.split(key, N_EP * EXPERTS)

    def one_block(subkey):
        return jax.random.permutation(subkey, TOK_DEV)[:SLOTS]
    orders = jax.vmap(one_block)(key_list)
    return orders.reshape(N_EP, EXPERTS, SLOTS).astype(jnp.int32)


def levels(rng, dims, cuts, smallest, high):
    loudness, own = 1.0, jax.random.fold_in(rng, 6)
    for axis_at, shards_of in cuts:
        heights = jnp.exp(jax.random.uniform(jax.random.fold_in(own, axis_at), (shards_of,), jnp.float32, smallest / len(cuts), high / len(cuts)))
        loudness = loudness * jnp.repeat(heights, dims[axis_at] // shards_of).reshape([-1 if axis == axis_at else 1 for axis in range(len(dims))])
    return loudness


def scatter_about(own_key, dims, spread, reach, cuts=(), kind=jnp.bfloat16):
    gain = levels(own_key, dims, cuts, -0.22, 0.18) if cuts else 1.0
    drawn = jax.random.normal(own_key, dims, jnp.float32) * spread * gain
    return jnp.minimum(jnp.maximum(drawn, -reach), reach).astype(kind)


def setup_inputs(seed: int = 0) -> dict:
    streams_of = jax.random.split(jax.random.key(seed), 11)
    tokens = scatter_about(streams_of[0], (TOKENS, D), 1.0, 6.0, ((0, 16), (1, 32)))
    picks = draw_picks(jax.random.fold_in(streams_of[10], 71), 0)
    pick_weights = jnp.clip(0.1 + 0.9 * jax.random.uniform(streams_of[2], (N_EP, EXPERTS, SLOTS), jnp.float32) ** levels(streams_of[2], (N_EP, EXPERTS, SLOTS), ((0, 16),), -0.2, 0.2), 0.1, 1.0)
    gate_weight = scatter_about(streams_of[3], (EXPERTS, FF, D), D ** -0.5, 0.09375, ((0, 16), (1, 32)))
    up_weight = scatter_about(streams_of[4], (EXPERTS, FF, D), D ** -0.5, 0.09375, ((0, 16), (1, 32)))
    down_weight = scatter_about(streams_of[5], (EXPERTS, FF, D), FF ** -0.5, 0.15625, ((0, 16), (2, 32)))
    dense_gate = scatter_about(streams_of[6], (DF, D), D ** -0.5, 0.09375, ((0, 32),))
    dense_up = scatter_about(streams_of[7], (DF, D), D ** -0.5, 0.09375, ((0, 32),))
    dense_down = scatter_about(streams_of[8], (DF, D), DF ** -0.5, 0.078125, ((0, 32),))
    branch_gate = scatter_about(streams_of[9], (D,), 1.5, 6.0, ((0, 32),), jnp.float32)
    return dict(tokens=tokens, picks=picks, pick_weights=pick_weights, gate_weight=gate_weight, up_weight=up_weight, down_weight=down_weight, dense_gate=dense_gate, dense_up=dense_up, dense_down=dense_down, branch_gate=branch_gate)


def reference(tokens, picks, pick_weights, gate_weight, up_weight, down_weight, dense_gate, dense_up, dense_down, branch_gate):
    offsets = (jnp.arange(N_EP, dtype=jnp.int32) * TOK_DEV)[:, None]
    mixture = jnp.zeros((TOKENS, D), jnp.float32)
    for expert in range(EXPERTS):
        row_index = (picks[:, expert, :] + offsets).reshape(-1).astype(jnp.int32)
        chosen = tokens[row_index]
        gate_value = jnp.dot(chosen, gate_weight[expert].T, preferred_element_type=jnp.float32)
        up_value = jnp.dot(chosen, up_weight[expert].T, preferred_element_type=jnp.float32)
        hidden = (jax.nn.silu(gate_value) * up_value).astype(jnp.bfloat16)
        result = jnp.dot(hidden, down_weight[expert], preferred_element_type=jnp.float32).astype(jnp.bfloat16)
        weights = pick_weights[:, expert, :].reshape(-1, 1)
        mixture = mixture.at[row_index].add(result.astype(jnp.float32) * weights)
    dense_gval = jnp.dot(tokens, dense_gate.T, preferred_element_type=jnp.float32)
    dense_uval = jnp.dot(tokens, dense_up.T, preferred_element_type=jnp.float32)
    dense_hidden = (jax.nn.silu(dense_gval) * dense_uval).astype(jnp.bfloat16)
    block_width = DF // N_TP
    dense_out = jnp.zeros((TOKENS, D), jnp.float32)
    for block_index in range(N_TP):
        lower = block_index * block_width
        partial_value = jnp.dot(dense_hidden[:, lower:lower + block_width], dense_down[lower:lower + block_width], preferred_element_type=jnp.float32)
        dense_out = dense_out + partial_value.astype(jnp.bfloat16).astype(jnp.float32)
    mixed = mixture + jax.nn.sigmoid(branch_gate)[None, :] * dense_out
    return mixed.astype(jnp.bfloat16)
```

```python
import functools

import jax
import jax.numpy as jnp
from jax import lax
from jax.experimental import pallas as pl
from jax.experimental.pallas import tpu as pltpu
from jax.sharding import Mesh
from jax.sharding import PartitionSpec as P

TP = ("za", "zb", "core")
LAST = (((1,), (1,)), ((), ()))
FIRST = (((0,), (0,)), ((), ()))
LANES = 128


def split_kernel(count, own_ref, *refs):
    ins, outs = refs[:-count], refs[-count:]
    own = own_ref[0]
    for k, out in enumerate(outs):
        for i, weight in enumerate(ins):
            for j in range(out.shape[2] // LANES):
                start = pl.multiple_of((j * count + (own ^ k)) * LANES, LANES)
                out[i, :, j * LANES : (j + 1) * LANES] = weight[:, pl.ds(start, LANES)]


def columns_for(own, count, *weights):
    rows, width = weights[0].shape
    return pl.pallas_call(
        functools.partial(split_kernel, count),
        out_shape=[
            jax.ShapeDtypeStruct((len(weights), rows, width // count), weights[0].dtype)
            for _ in range(count)
        ],
        in_specs=[pl.BlockSpec(memory_space=pltpu.SMEM)]
        + [pl.BlockSpec(memory_space=pltpu.VMEM)] * len(weights),
        out_specs=[pl.BlockSpec(memory_space=pltpu.VMEM)] * count,
        name=f"columns_{count}_{rows}",
    )(own.reshape(1), *weights)


def swap(x, axes, size, k):
    return lax.ppermute(x, axes, [(i, i ^ k) for i in range(size)])


def dot(a, b, dims):
    return lax.dot_general(a, b, dims, preferred_element_type=jnp.float32)


def per_device(
    tokens,
    picks,
    pick_weights,
    gate_weight,
    up_weight,
    down_weight,
    dense_gate,
    dense_up,
    dense_down,
    branch_gate,
):
    core = lax.axis_index("core")
    quad = lax.axis_index("zb") * 2 + core
    rows, width = tokens.shape
    experts, slots = picks.shape[1:]
    n_za = lax.axis_size("za")
    n_z = 2 * n_za
    hid = gate_weight.shape[1]
    dense_hid = dense_gate.shape[0]

    with jax.named_scope("gather"):
        tiles = lax.all_gather(tokens, ("za", "zb"), axis=0, tiled=False)
        mine = jnp.moveaxis(tiles, 0, 1).reshape(rows, n_z * width)

    with jax.named_scope("pick"):
        chosen = picks.reshape(-1)
        pick_matrix = (
            lax.broadcasted_iota(jnp.int32, (experts * slots, rows), 1) == chosen[:, None]
        ).astype(jnp.bfloat16)
        picked = dot(pick_matrix, mine, (((1,), (0,)), ((), ()))).astype(jnp.bfloat16)
        picked = picked.reshape(experts, slots, n_z * width)
    with jax.named_scope("ship"):
        landed = lax.all_to_all(picked, "ep", split_axis=0, concat_axis=0, tiled=True)
        landed = landed.reshape(-1, n_z * width)

    with jax.named_scope("dense_tokens"):
        theirs = swap(tiles, "core", 2, 1)
        theirs = jnp.moveaxis(theirs, 0, 1).reshape(rows, n_z * width)
    with jax.named_scope("dense_weights"):
        dense_own, dense_other = columns_for(core, 2, dense_gate, dense_up)
        down_0, down_1, down_2, down_3 = columns_for(quad, 4, dense_down)
        down_came = swap(jnp.concatenate([down_1, down_3], 0), "core", 2, 1)
    with jax.named_scope("dense_up"):
        dense_own = dense_own.reshape(2 * dense_hid, -1)
        dense_other = dense_other.reshape(2 * dense_hid, -1)
        dense_gu = dot(dense_own, mine, LAST) + dot(dense_other, theirs, LAST)
        dense_hidden = jax.nn.silu(dense_gu[:dense_hid]) * dense_gu[dense_hid:]
        dense_hidden = dense_hidden.astype(jnp.bfloat16)
        dense_came = swap(dense_hidden, "core", 2, 1)
    with jax.named_scope("dense_down"):
        keep = dot(dense_hidden, down_0[0], FIRST) + dot(dense_came, down_came[0], FIRST)
        give = dot(dense_hidden, down_2[0], FIRST) + dot(dense_came, down_came[1], FIRST)
        keep, give = (
            jnp.moveaxis(x.astype(jnp.bfloat16).reshape(rows, n_za, width), 1, 0)
            for x in (keep, give)
        )
    with jax.named_scope("dense_pair"):
        came = swap(give, "zb", 2, 1)
    with jax.named_scope("dense_sum"):
        pair = (keep.astype(jnp.float32) + came.astype(jnp.float32)).astype(jnp.bfloat16)
        pieces = lax.all_to_all(pair, "za", split_axis=0, concat_axis=0, tiled=True)

    with jax.named_scope("expert_weights"):
        gu_own, gu_other = columns_for(core, 2, gate_weight[0], up_weight[0])
        gu_came = swap(gu_other, "core", 2, 1)
        gu_own = gu_own.reshape(2 * hid, -1)
        gu_came = gu_came.reshape(2 * hid, -1)
        down = down_weight[0].reshape(n_za, 4, hid, width)
        turned = []
        for k in range(4):
            part = lax.dynamic_index_in_dim(down, quad ^ k, 1, keepdims=False)
            part = part.reshape(n_za * hid, width)
            turned.append(swap(part, ("zb", "core"), 4, k) if k else part)
        turned = jnp.stack(turned)
        columns = [
            lax.dynamic_index_in_dim(turned, quad ^ q, 0, keepdims=False) for q in range(4)
        ]

    with jax.named_scope("expert_up"):
        part_other = dot(gu_came, landed, LAST)
        part_came = swap(part_other, "core", 2, 1)
        gate_up = dot(gu_own, landed, LAST) + part_came
        hidden = (jax.nn.silu(gate_up[:hid]) * gate_up[hid:]).astype(jnp.bfloat16)

    with jax.named_scope("hidden_gather"):
        units = lax.all_gather(hidden, "za", axis=0, tiled=True)
    with jax.named_scope("expert_down"):
        outgoing = jnp.stack([dot(units, c, FIRST).astype(jnp.bfloat16) for c in columns])
        outgoing = outgoing.reshape(4 * experts, slots, width)
    with jax.named_scope("back"):
        back = lax.all_to_all(
            outgoing, ("zb", "core", "ep"), split_axis=0, concat_axis=0, tiled=True
        )

    with jax.named_scope("mixture"):
        token = lax.broadcasted_iota(jnp.int32, (rows, experts * slots), 0)
        spread = jnp.where(token == chosen[None, :], pick_weights.reshape(1, -1), 0.0)
        high = spread.astype(jnp.bfloat16)
        low = (spread - high.astype(jnp.float32)).astype(jnp.bfloat16)
        came = back.reshape(4 * experts * slots, width)
        plain = (((1,), (0,)), ((), ()))
        mixture = dot(jnp.tile(high, (1, 4)), came, plain) + dot(jnp.tile(low, (1, 4)), came, plain)
        dense_out = jnp.sum(pieces.astype(jnp.float32), axis=0)
        mixed = mixture + jax.nn.sigmoid(branch_gate)[None, :] * dense_out
    return mixed.astype(jnp.bfloat16)


def solution(mesh):
    split = Mesh(
        mesh.devices.reshape(mesh.shape["ep"], mesh.shape["tp"] // 4, 2, 2),
        ("ep", "za", "zb", "core"),
    )
    placed = (
        P("ep", TP),
        P("ep", None, None),
        P("ep", None, None),
        P("ep", TP, None),
        P("ep", TP, None),
        P("ep", None, TP),
        P(TP, None),
        P(TP, None),
        P(TP, None),
        P(TP),
    )
    return jax.shard_map(
        per_device, mesh=split, in_specs=placed, out_specs=P("ep", TP), check_vma=False
    )
```

```python
import jax
import jax.numpy as jnp
from jax import lax
from jax.experimental import pallas as pl
from jax.experimental.pallas import tpu as pltpu
from jax.sharding import Mesh
from jax.sharding import PartitionSpec as P


TP = ("za", "zb", "core")
LAST = (((1,), (1,)), ((), ()))
FIRST = (((0,), (0,)), ((), ()))
PLAIN = (((1,), (0,)), ((), ()))
LANES = 128


def expert_kernel(own_ref, gate, up, down, *outs):
    own = own_ref[0]
    for k, out in enumerate(outs):
        for j in range(out.shape[2] // LANES):
            tile = j * 4 + (own ^ k)
            start = pl.multiple_of(tile * LANES, LANES)
            at = slice(j * LANES, (j + 1) * LANES)
            out[0, :, at] = gate[:, pl.ds(start, LANES)]
            out[1, :, at] = up[:, pl.ds(start, LANES)]
            out[2, :, at] = down[tile]


def dense_kernel(own_ref, gate, up, *outs):
    own = own_ref[0]
    rows = gate.shape[0]
    for k, out in enumerate(outs):
        for j in range(out.shape[1] // LANES):
            start = pl.multiple_of((j * 4 + (own ^ k)) * LANES, LANES)
            at = slice(j * LANES, (j + 1) * LANES)
            out[:rows, at] = gate[:, pl.ds(start, LANES)]
            out[rows:, at] = up[:, pl.ds(start, LANES)]


def down_kernel(own_ref, weight, *outs):
    core = own_ref[0] & 1
    for k, out in enumerate(outs):
        for j in range(out.shape[1] // LANES):
            start = pl.multiple_of((j * 2 + (core ^ k)) * LANES, LANES)
            out[:, j * LANES : (j + 1) * LANES] = weight[:, pl.ds(start, LANES)]


def split_up(kernel, own, outs, *weights):
    return pl.pallas_call(
        kernel,
        out_shape=[jax.ShapeDtypeStruct(shape, jnp.bfloat16) for shape in outs],
        in_specs=[pl.BlockSpec(memory_space=pltpu.SMEM)]
        + [pl.BlockSpec(memory_space=pltpu.VMEM)] * len(weights),
        out_specs=[pl.BlockSpec(memory_space=pltpu.VMEM)] * len(outs),
    )(own.reshape(1), *weights)


def swap(x, axes, size, k):
    return lax.ppermute(x, axes, [(i, i ^ k) for i in range(size)])


def flat(tiles):
    return jnp.moveaxis(tiles, 0, 1).reshape(tiles.shape[1], -1)


def dot(a, b, dims):
    return lax.dot_general(a, b, dims, preferred_element_type=jnp.float32)


def per_device(
    tokens,
    picks,
    pick_weights,
    gate_weight,
    up_weight,
    down_weight,
    dense_gate,
    dense_up,
    dense_down,
    branch_gate,
):
    quad = lax.axis_index("zb") * 2 + lax.axis_index("core")
    rows, width = tokens.shape
    experts, slots = picks.shape[1:]
    n_za = lax.axis_size("za")
    part = n_za * width
    hid = gate_weight.shape[1]
    dense_hid = dense_gate.shape[0]

    tiles = lax.all_to_all(
        jnp.broadcast_to(tokens, (n_za, rows, width)), "za", split_axis=0, concat_axis=0, tiled=True
    )
    mine = flat(tiles)

    down = down_weight[0].reshape(n_za * 4, hid, width)
    packs = split_up(expert_kernel, quad, [(3, hid, part)] * 4, gate_weight[0], up_weight[0], down)
    own, near, far, across = packs
    near = swap(near, "core", 2, 1)
    far = swap(far, "zb", 2, 1)
    across = swap(across, ("zb", "core"), 4, 3)
    packs = [own, near, far, across]
    gu = [x[:2].reshape(2 * hid, part) for x in packs]
    turned = jnp.stack([x[2] for x in packs]).reshape(4, hid, n_za, width)
    turned = jnp.moveaxis(turned, 2, 1).reshape(4, n_za * hid, width)
    columns = [
        lax.dynamic_index_in_dim(turned, quad ^ q, 0, keepdims=False) for q in range(4)
    ]
    down_keep, down_give = split_up(
        down_kernel, quad, [(dense_hid, 2 * part)] * 2, dense_down
    )
    down_came = swap(down_give, "core", 2, 1)
    dense_gu_weights = split_up(
        dense_kernel, quad, [(2 * dense_hid, part)] * 4, dense_gate, dense_up
    )

    chosen = picks.reshape(-1)
    pick_matrix = (
        lax.broadcasted_iota(jnp.int32, (experts * slots, rows), 1) == chosen[:, None]
    ).astype(jnp.bfloat16)
    picked = dot(pick_matrix, mine, PLAIN).astype(jnp.bfloat16)
    picked = picked.reshape(experts, slots, part)
    landed = lax.all_to_all(picked, "ep", split_axis=0, concat_axis=0, tiled=True)
    landed = landed.reshape(-1, part)

    tiles_z = swap(tiles, "zb", 2, 1)
    sets = [tiles, swap(tiles, "core", 2, 1), tiles_z, swap(tiles_z, "core", 2, 1)]
    dense_gu = sum(dot(w, flat(t), LAST) for w, t in zip(dense_gu_weights, sets))
    dense_hidden = jax.nn.silu(dense_gu[:dense_hid]) * dense_gu[dense_hid:]
    dense_hidden = dense_hidden.astype(jnp.bfloat16)
    dense_came = swap(dense_hidden, "core", 2, 1)
    wide = dot(dense_hidden, down_keep, FIRST) + dot(dense_came, down_came, FIRST)
    wide = wide.astype(jnp.bfloat16).reshape(rows, 2 * n_za, width)
    dense_out = lax.psum_scatter(
        jnp.moveaxis(wide, 1, 0), ("za", "zb"), scatter_dimension=0, tiled=False
    )

    odd = dot(jnp.concatenate([gu[1], gu[3]], 0), landed, LAST)
    odd_came = swap(odd, "core", 2, 1)
    even = dot(jnp.concatenate([gu[0], gu[2]], 0), landed, LAST) + odd_came
    far = swap(even[2 * hid :].astype(jnp.bfloat16), "zb", 2, 1)
    gate_up = even[: 2 * hid] + far.astype(jnp.float32)
    hidden = (jax.nn.silu(gate_up[:hid]) * gate_up[hid:]).astype(jnp.bfloat16)

    units = lax.all_gather(hidden, "za", axis=0, tiled=True)
    outgoing = jnp.stack([dot(units, c, FIRST).astype(jnp.bfloat16) for c in columns])
    outgoing = outgoing.reshape(4 * experts, slots, width)
    back = lax.all_to_all(outgoing, ("zb", "core", "ep"), split_axis=0, concat_axis=0, tiled=True)

    token = lax.broadcasted_iota(jnp.int32, (rows, experts * slots), 0)
    spread = jnp.where(token == chosen[None, :], pick_weights.reshape(1, -1), 0.0)
    spread = jnp.tile(spread.astype(jnp.bfloat16), (1, 4))
    mixture = dot(spread, back.reshape(4 * experts * slots, width), PLAIN)
    mixed = mixture + jax.nn.sigmoid(branch_gate)[None, :] * dense_out.astype(jnp.float32)
    return mixed.astype(jnp.bfloat16)


def solution(mesh):
    split = Mesh(
        mesh.devices.reshape(mesh.shape["ep"], mesh.shape["tp"] // 4, 2, 2),
        ("ep", "za", "zb", "core"),
    )
    placed = (
        P("ep", TP),
        P("ep", None, None),
        P("ep", None, None),
        P("ep", TP, None),
        P("ep", TP, None),
        P("ep", None, TP),
        P(TP, None),
        P(TP, None),
        P(TP, None),
        P(TP),
    )

    return jax.shard_map(
        per_device, mesh=split, in_specs=placed, out_specs=P("ep", TP), check_vma=False
    )
```

```python
import jax
import jax.numpy as jnp
from jax import lax
from jax.experimental import pallas as pl
from jax.experimental.pallas import tpu as pltpu
from jax.sharding import Mesh
from jax.sharding import PartitionSpec as P


TP = ("za", "zb", "core")
LAST = (((1,), (1,)), ((), ()))
FIRST = (((0,), (0,)), ((), ()))
PLAIN = (((1,), (0,)), ((), ()))
LANES = 128


def expert_kernel(own_ref, gate, up, down, gu_own, gu_far, gu_near, own_out, far_out, near_out):
    own = own_ref[0]
    pairs = (gu_own, gu_near.at[0], gu_far, gu_near.at[1])
    turns = (own_out, near_out.at[0], far_out, near_out.at[1])
    for k in range(4):
        for j in range(own_out.shape[0]):
            tile = j * 4 + (own ^ k)
            start = pl.multiple_of(tile * LANES, LANES)
            at = slice(j * LANES, (j + 1) * LANES)
            pairs[k][0, :, at] = gate[:, pl.ds(start, LANES)]
            pairs[k][1, :, at] = up[:, pl.ds(start, LANES)]
            turns[k][j] = down[tile]


def dense_kernel(own_ref, gate, up, keep, give):
    own = own_ref[0]
    rows = gate.shape[0]
    for k in range(4):
        out = give if k % 2 else keep
        for j in range(out.shape[2] // LANES):
            start = pl.multiple_of((j * 4 + (own ^ k)) * LANES, LANES)
            at = slice(j * LANES, (j + 1) * LANES)
            out[k // 2, :rows, at] = gate[:, pl.ds(start, LANES)]
            out[k // 2, rows:, at] = up[:, pl.ds(start, LANES)]


def down_kernel(own_ref, weight, *outs):
    core = own_ref[0] & 1
    for k, out in enumerate(outs):
        for j in range(out.shape[1] // LANES):
            start = pl.multiple_of((j * 2 + (core ^ k)) * LANES, LANES)
            out[:, j * LANES : (j + 1) * LANES] = weight[:, pl.ds(start, LANES)]


def split_up(kernel, own, outs, *weights):
    return pl.pallas_call(
        kernel,
        out_shape=[jax.ShapeDtypeStruct(shape, jnp.bfloat16) for shape in outs],
        in_specs=[pl.BlockSpec(memory_space=pltpu.SMEM)]
        + [pl.BlockSpec(memory_space=pltpu.VMEM)] * len(weights),
        out_specs=[pl.BlockSpec(memory_space=pltpu.VMEM)] * len(outs),
    )(own.reshape(1), *weights)


def swap(x, axes, size, k):
    return lax.ppermute(x, axes, [(i, i ^ k) for i in range(size)])


def flat(tiles):
    return jnp.moveaxis(tiles, 0, 1).reshape(tiles.shape[1], -1)


def dot(a, b, dims):
    return lax.dot_general(a, b, dims, preferred_element_type=jnp.float32)


def per_device(
    tokens,
    picks,
    pick_weights,
    gate_weight,
    up_weight,
    down_weight,
    dense_gate,
    dense_up,
    dense_down,
    branch_gate,
):
    quad = lax.axis_index("zb") * 2 + lax.axis_index("core")
    rows, width = tokens.shape
    experts, slots = picks.shape[1:]
    n_za = lax.axis_size("za")
    part = n_za * width
    hid = gate_weight.shape[1]
    dense_hid = dense_gate.shape[0]

    tiles = lax.all_to_all(
        jnp.broadcast_to(tokens, (n_za, rows, width)), "za", split_axis=0, concat_axis=0, tiled=True
    )
    mine = flat(tiles)

    down = down_weight[0].reshape(n_za * 4, hid, width)
    pair, turn = (2, hid, part), (n_za, hid, width)
    gu_own, gu_far, gu_near, turn_own, turn_far, turn_near = split_up(
        expert_kernel,
        quad,
        [pair, pair, (2, *pair), turn, turn, (2, *turn)],
        gate_weight[0],
        up_weight[0],
        down,
    )
    gu_near = swap(gu_near, "core", 2, 1)
    relay = jnp.stack([gu_far, gu_near[1]])
    gu_far = swap(relay, "zb", 2, 1)
    gu = [gu_own, gu_near[0], gu_far[0], gu_far[1]]
    gu = [x.reshape(2 * hid, part) for x in gu]
    turn_near = swap(turn_near, "core", 2, 1)
    turn_far = swap(jnp.stack([turn_far, turn_near[1]]), "zb", 2, 1)
    turned = jnp.stack([turn_own, turn_near[0], turn_far[0], turn_far[1]])
    turned = turned.reshape(4, n_za * hid, width)
    columns = [
        lax.dynamic_index_in_dim(turned, quad ^ q, 0, keepdims=False) for q in range(4)
    ]
    dense_keep, dense_give = split_up(
        dense_kernel, quad, [(2, 2 * dense_hid, part)] * 2, dense_gate, dense_up
    )
    down_keep, down_give = split_up(
        down_kernel, quad, [(dense_hid, 2 * part)] * 2, dense_down
    )
    dense_came = swap(dense_give, "core", 2, 1)
    down_came = swap(down_give, "core", 2, 1)

    chosen = picks.reshape(-1)
    pick_matrix = (
        lax.broadcasted_iota(jnp.int32, (experts * slots, rows), 1) == chosen[:, None]
    ).astype(jnp.bfloat16)
    picked = dot(pick_matrix, mine, PLAIN).astype(jnp.bfloat16)
    picked = picked.reshape(experts, slots, part)
    landed = lax.all_to_all(picked, "ep", split_axis=0, concat_axis=0, tiled=True)
    landed = landed.reshape(-1, part)

    tiles_far = swap(tiles, "zb", 2, 1)
    firsts = [dot(w[0], mine, LAST) for w in (dense_keep, dense_came)]
    firsts = lax.optimization_barrier(firsts)
    theirs = flat(tiles_far)
    own_part, pair_part = (
        first + dot(w[1], theirs, LAST) for first, w in zip(firsts, (dense_keep, dense_came))
    )
    came_part = swap(jnp.stack([pair_part, own_part]), "core", 2, 1)
    dense_hidden = []
    for gu_sum in (own_part + came_part[0], pair_part + came_part[1]):
        value = jax.nn.silu(gu_sum[:dense_hid]) * gu_sum[dense_hid:]
        dense_hidden.append(value.astype(jnp.bfloat16))
    wide = dot(dense_hidden[0], down_keep, FIRST) + dot(dense_hidden[1], down_came, FIRST)
    wide = wide.astype(jnp.bfloat16).reshape(rows, 2 * n_za, width)
    dense_out = lax.psum_scatter(
        jnp.moveaxis(wide, 1, 0), ("za", "zb"), scatter_dimension=0, tiled=False
    )

    odd = dot(jnp.concatenate([gu[1], gu[3]], 0), landed, LAST)
    odd_came = swap(odd, "core", 2, 1)
    even = dot(jnp.concatenate([gu[0], gu[2]], 0), landed, LAST) + odd_came
    far = swap(even[2 * hid :].astype(jnp.bfloat16), "zb", 2, 1)
    gate_up = even[: 2 * hid] + far.astype(jnp.float32)
    hidden = (jax.nn.silu(gate_up[:hid]) * gate_up[hid:]).astype(jnp.bfloat16)

    units = lax.all_gather(hidden, "za", axis=0, tiled=True)
    outgoing = jnp.stack([dot(units, c, FIRST).astype(jnp.bfloat16) for c in columns])
    outgoing = outgoing.reshape(4 * experts, slots, width)
    back = lax.all_to_all(outgoing, ("zb", "core", "ep"), split_axis=0, concat_axis=0, tiled=True)

    token = lax.broadcasted_iota(jnp.int32, (rows, experts * slots), 0)
    spread = jnp.where(token == chosen[None, :], pick_weights.reshape(1, -1), 0.0)
    spread = jnp.tile(spread.astype(jnp.bfloat16), (1, 4))
    mixture = dot(spread, back.reshape(4 * experts * slots, width), PLAIN)
    mixed = mixture + jax.nn.sigmoid(branch_gate)[None, :] * dense_out.astype(jnp.float32)
    return mixed.astype(jnp.bfloat16)


def solution(mesh):
    split = Mesh(
        mesh.devices.reshape(mesh.shape["ep"], mesh.shape["tp"] // 4, 2, 2),
        ("ep", "za", "zb", "core"),
    )
    placed = (
        P("ep", TP),
        P("ep", None, None),
        P("ep", None, None),
        P("ep", TP, None),
        P("ep", TP, None),
        P("ep", None, TP),
        P(TP, None),
        P(TP, None),
        P(TP, None),
        P(TP),
    )

    return jax.shard_map(
        per_device, mesh=split, in_specs=placed, out_specs=P("ep", TP), check_vma=False
    )
```

```python
import jax
import jax.numpy as jnp
from jax import lax
from jax.experimental import pallas as pl
from jax.experimental.pallas import tpu as pltpu
from jax.sharding import Mesh
from jax.sharding import PartitionSpec as P


TP = ("za", "zb", "core")
LAST = (((1,), (1,)), ((), ()))
FIRST = (((0,), (0,)), ((), ()))
PLAIN = (((1,), (0,)), ((), ()))
LANES = 128


def expert_kernel(own_ref, gate, up, down, gu_own, turn_own, far, near):
    own = own_ref[0]
    packs = (None, near.at[0], far, near.at[1])
    for k, pack in enumerate(packs):
        for j in range(turn_own.shape[0]):
            tile = j * 4 + (own ^ k)
            start = pl.multiple_of(tile * LANES, LANES)
            at = slice(j * LANES, (j + 1) * LANES)
            pair = pack if k else gu_own
            pair[0, :, at] = gate[:, pl.ds(start, LANES)]
            pair[1, :, at] = up[:, pl.ds(start, LANES)]
            if k:
                pack[2, :, at] = down[tile]
            else:
                turn_own[j] = down[tile]


def dense_kernel(own_ref, gate, up, keep, give):
    own = own_ref[0]
    rows = gate.shape[0]
    for k in range(4):
        out = give if k % 2 else keep
        for j in range(out.shape[2] // LANES):
            start = pl.multiple_of((j * 4 + (own ^ k)) * LANES, LANES)
            at = slice(j * LANES, (j + 1) * LANES)
            out[k // 2, :rows, at] = gate[:, pl.ds(start, LANES)]
            out[k // 2, rows:, at] = up[:, pl.ds(start, LANES)]


def down_kernel(own_ref, weight, *outs):
    core = own_ref[0] & 1
    for k, out in enumerate(outs):
        for j in range(out.shape[1] // LANES):
            start = pl.multiple_of((j * 2 + (core ^ k)) * LANES, LANES)
            out[:, j * LANES : (j + 1) * LANES] = weight[:, pl.ds(start, LANES)]


def split_up(kernel, own, outs, *weights):
    return pl.pallas_call(
        kernel,
        out_shape=[jax.ShapeDtypeStruct(shape, jnp.bfloat16) for shape in outs],
        in_specs=[pl.BlockSpec(memory_space=pltpu.SMEM)]
        + [pl.BlockSpec(memory_space=pltpu.VMEM)] * len(weights),
        out_specs=[pl.BlockSpec(memory_space=pltpu.VMEM)] * len(outs),
    )(own.reshape(1), *weights)


def swap(x, axes, size, k):
    return lax.ppermute(x, axes, [(i, i ^ k) for i in range(size)])


def flat(tiles):
    return jnp.moveaxis(tiles, 0, 1).reshape(tiles.shape[1], -1)


def dot(a, b, dims):
    return lax.dot_general(a, b, dims, preferred_element_type=jnp.float32)


def per_device(
    tokens,
    picks,
    pick_weights,
    gate_weight,
    up_weight,
    down_weight,
    dense_gate,
    dense_up,
    dense_down,
    branch_gate,
):
    quad = lax.axis_index("zb") * 2 + lax.axis_index("core")
    rows, width = tokens.shape
    experts, slots = picks.shape[1:]
    n_za = lax.axis_size("za")
    part = n_za * width
    hid = gate_weight.shape[1]
    dense_hid = dense_gate.shape[0]

    tiles = lax.all_to_all(
        jnp.broadcast_to(tokens, (n_za, rows, width)), "za", split_axis=0, concat_axis=0, tiled=True
    )
    mine = flat(tiles)

    down = down_weight[0].reshape(n_za * 4, hid, width)
    pack = (3, hid, part)
    gu_own, turn_own, far, near = split_up(
        expert_kernel,
        quad,
        [(2, hid, part), (n_za, hid, width), pack, (2, *pack)],
        gate_weight[0],
        up_weight[0],
        down,
    )
    near = swap(near, "core", 2, 1)
    far = jnp.stack([far, near[1]])
    far = swap(far, "zb", 2, 1)
    gu = [gu_own, near[0, :2], far[0, :2], far[1, :2]]
    gu = [x.reshape(2 * hid, part) for x in gu]
    turned = [
        jnp.moveaxis(x.reshape(hid, n_za, width), 1, 0)
        for x in (near[0, 2], far[0, 2], far[1, 2])
    ]
    turned = jnp.stack([turn_own, *turned]).reshape(4, n_za * hid, width)
    columns = [
        lax.dynamic_index_in_dim(turned, quad ^ q, 0, keepdims=False) for q in range(4)
    ]
    dense_keep, dense_give = split_up(
        dense_kernel, quad, [(2, 2 * dense_hid, part)] * 2, dense_gate, dense_up
    )
    down_keep, down_give = split_up(
        down_kernel, quad, [(dense_hid, 2 * part)] * 2, dense_down
    )
    dense_came = swap(dense_give, "core", 2, 1)
    down_came = swap(down_give, "core", 2, 1)

    chosen = picks.reshape(-1)
    pick_matrix = (
        lax.broadcasted_iota(jnp.int32, (experts * slots, rows), 1) == chosen[:, None]
    ).astype(jnp.bfloat16)
    picked = dot(pick_matrix, mine, PLAIN).astype(jnp.bfloat16)
    picked = picked.reshape(experts, slots, part)
    landed = lax.all_to_all(picked, "ep", split_axis=0, concat_axis=0, tiled=True)
    landed = landed.reshape(-1, part)

    tiles_far = swap(tiles, "zb", 2, 1)
    firsts = [dot(w[0], mine, LAST) for w in (dense_keep, dense_came)]
    firsts = lax.optimization_barrier(firsts)
    theirs = flat(tiles_far)
    own_part, pair_part = (
        first + dot(w[1], theirs, LAST) for first, w in zip(firsts, (dense_keep, dense_came))
    )
    came_part = swap(jnp.stack([pair_part, own_part]), "core", 2, 1)
    dense_hidden = []
    for gu_sum in (own_part + came_part[0], pair_part + came_part[1]):
        value = jax.nn.silu(gu_sum[:dense_hid]) * gu_sum[dense_hid:]
        dense_hidden.append(value.astype(jnp.bfloat16))
    wide = dot(dense_hidden[0], down_keep, FIRST) + dot(dense_hidden[1], down_came, FIRST)
    wide = wide.astype(jnp.bfloat16).reshape(rows, 2 * n_za, width)
    dense_out = lax.psum_scatter(
        jnp.moveaxis(wide, 1, 0), ("za", "zb"), scatter_dimension=0, tiled=False
    )

    odd = dot(jnp.concatenate([gu[1], gu[3]], 0), landed, LAST)
    odd_came = swap(odd, "core", 2, 1)
    even = dot(jnp.concatenate([gu[0], gu[2]], 0), landed, LAST) + odd_came
    far = swap(even[2 * hid :].astype(jnp.bfloat16), "zb", 2, 1)
    gate_up = even[: 2 * hid] + far.astype(jnp.float32)
    hidden = (jax.nn.silu(gate_up[:hid]) * gate_up[hid:]).astype(jnp.bfloat16)

    units = lax.all_gather(hidden, "za", axis=0, tiled=True)
    outgoing = jnp.stack([dot(units, c, FIRST).astype(jnp.bfloat16) for c in columns])
    outgoing = outgoing.reshape(4 * experts, slots, width)
    back = lax.all_to_all(outgoing, ("zb", "core", "ep"), split_axis=0, concat_axis=0, tiled=True)

    token = lax.broadcasted_iota(jnp.int32, (rows, experts * slots), 0)
    spread = jnp.where(token == chosen[None, :], pick_weights.reshape(1, -1), 0.0)
    parts = back.reshape(4, experts * slots, width).astype(jnp.float32)
    results = jnp.sum(parts, axis=0).astype(jnp.bfloat16)
    mixture = dot(spread.astype(jnp.bfloat16), results, PLAIN)
    mixed = mixture + jax.nn.sigmoid(branch_gate)[None, :] * dense_out.astype(jnp.float32)
    return mixed.astype(jnp.bfloat16)


def solution(mesh):
    split = Mesh(
        mesh.devices.reshape(mesh.shape["ep"], mesh.shape["tp"] // 4, 2, 2),
        ("ep", "za", "zb", "core"),
    )
    placed = (
        P("ep", TP),
        P("ep", None, None),
        P("ep", None, None),
        P("ep", TP, None),
        P("ep", TP, None),
        P("ep", None, TP),
        P(TP, None),
        P(TP, None),
        P(TP, None),
        P(TP),
    )

    return jax.shard_map(
        per_device, mesh=split, in_specs=placed, out_specs=P("ep", TP), check_vma=False
    )
```

```python
import jax
import jax.numpy as jnp
from jax import lax
from jax.experimental import pallas as pl
from jax.experimental.pallas import tpu as pltpu
from jax.sharding import Mesh
from jax.sharding import PartitionSpec as P


TP = ("za", "zb", "core")
LAST = (((1,), (1,)), ((), ()))
FIRST = (((0,), (0,)), ((), ()))
PLAIN = (((1,), (0,)), ((), ()))
LANES = 128


def expert_kernel(own_ref, gate, up, down, gu_own, gu_far, gu_near, own_out, far_out, near_out):
    own = own_ref[0]
    pairs = (gu_own, gu_near.at[0], gu_far, gu_near.at[1])
    turns = (own_out, near_out.at[0], far_out, near_out.at[1])
    for k in range(4):
        for j in range(own_out.shape[0]):
            tile = j * 4 + (own ^ k)
            start = pl.multiple_of(tile * LANES, LANES)
            at = slice(j * LANES, (j + 1) * LANES)
            pairs[k][0, :, at] = gate[:, pl.ds(start, LANES)]
            pairs[k][1, :, at] = up[:, pl.ds(start, LANES)]
            turns[k][j] = down[tile]


def dense_kernel(own_ref, gate, up, keep, give):
    own = own_ref[0]
    rows = gate.shape[0]
    for k in range(4):
        out = give if k % 2 else keep
        for j in range(out.shape[2] // LANES):
            start = pl.multiple_of((j * 4 + (own ^ k)) * LANES, LANES)
            at = slice(j * LANES, (j + 1) * LANES)
            out[k // 2, :rows, at] = gate[:, pl.ds(start, LANES)]
            out[k // 2, rows:, at] = up[:, pl.ds(start, LANES)]


def down_kernel(own_ref, weight, *outs):
    core = own_ref[0] & 1
    for k, out in enumerate(outs):
        for j in range(out.shape[1] // LANES):
            start = pl.multiple_of((j * 2 + (core ^ k)) * LANES, LANES)
            out[:, j * LANES : (j + 1) * LANES] = weight[:, pl.ds(start, LANES)]


def split_up(kernel, own, outs, *weights):
    return pl.pallas_call(
        kernel,
        out_shape=[jax.ShapeDtypeStruct(shape, jnp.bfloat16) for shape in outs],
        in_specs=[pl.BlockSpec(memory_space=pltpu.SMEM)]
        + [pl.BlockSpec(memory_space=pltpu.VMEM)] * len(weights),
        out_specs=[pl.BlockSpec(memory_space=pltpu.VMEM)] * len(outs),
    )(own.reshape(1), *weights)


def swap(x, axes, size, k):
    return lax.ppermute(x, axes, [(i, i ^ k) for i in range(size)])


def flat(tiles):
    return jnp.moveaxis(tiles, 0, 1).reshape(tiles.shape[1], -1)


def dot(a, b, dims):
    return lax.dot_general(a, b, dims, preferred_element_type=jnp.float32)


def per_device(
    tokens,
    picks,
    pick_weights,
    gate_weight,
    up_weight,
    down_weight,
    dense_gate,
    dense_up,
    dense_down,
    branch_gate,
):
    quad = lax.axis_index("zb") * 2 + lax.axis_index("core")
    rows, width = tokens.shape
    experts, slots = picks.shape[1:]
    n_za = lax.axis_size("za")
    part = n_za * width
    hid = gate_weight.shape[1]
    dense_hid = dense_gate.shape[0]

    tiles = lax.all_to_all(
        jnp.broadcast_to(tokens, (n_za, rows, width)), "za", split_axis=0, concat_axis=0, tiled=True
    )
    mine = flat(tiles)

    down = down_weight[0].reshape(n_za * 4, hid, width)
    pair, turn = (2, hid, part), (n_za, hid, width)
    gu_own, gu_far, gu_near, turn_own, turn_far, turn_near = split_up(
        expert_kernel,
        quad,
        [pair, pair, (2, *pair), turn, turn, (2, *turn)],
        gate_weight[0],
        up_weight[0],
        down,
    )
    gu_near = swap(gu_near, "core", 2, 1)
    relay = jnp.stack([gu_far, gu_near[1]])
    gu_far = swap(relay, "zb", 2, 1)
    gu = [gu_own, gu_near[0], gu_far[0], gu_far[1]]
    gu = [x.reshape(2 * hid, part) for x in gu]
    turn_near = swap(turn_near, "core", 2, 1)
    turn_far = swap(jnp.stack([turn_far, turn_near[1]]), "zb", 2, 1)
    turned = jnp.stack([turn_own, turn_near[0], turn_far[0], turn_far[1]])
    turned = turned.reshape(4, n_za * hid, width)
    columns = jnp.stack(
        [lax.dynamic_index_in_dim(turned, quad ^ q, 0, keepdims=False) for q in range(4)]
    )
    dense_keep, dense_give = split_up(
        dense_kernel, quad, [(2, 2 * dense_hid, part)] * 2, dense_gate, dense_up
    )
    dense_came = swap(dense_give, "core", 2, 1)

    down_keep, down_give = split_up(
        down_kernel, quad, [(dense_hid, 2 * part)] * 2, dense_down
    )
    down_came = swap(down_give, "core", 2, 1)

    chosen = picks.reshape(-1)
    pick_matrix = (
        lax.broadcasted_iota(jnp.int32, (experts * slots, rows), 1) == chosen[:, None]
    ).astype(jnp.bfloat16)
    picked = dot(pick_matrix, mine, PLAIN).astype(jnp.bfloat16)
    picked = picked.reshape(experts, slots, part)
    landed = lax.all_to_all(picked, "ep", split_axis=0, concat_axis=0, tiled=True)
    landed = landed.reshape(-1, part)

    tiles_far = swap(tiles, "zb", 2, 1)
    firsts = [dot(w[0], mine, LAST) for w in (dense_keep, dense_came)]
    firsts = lax.optimization_barrier(firsts)
    theirs = flat(tiles_far)
    own_part, pair_part = (
        first + dot(w[1], theirs, LAST) for first, w in zip(firsts, (dense_keep, dense_came))
    )
    came_part = swap(jnp.stack([pair_part, own_part]), "core", 2, 1)
    dense_hidden = []
    for gu_sum in (own_part + came_part[0], pair_part + came_part[1]):
        value = jax.nn.silu(gu_sum[:dense_hid]) * gu_sum[dense_hid:]
        dense_hidden.append(value.astype(jnp.bfloat16))
    wide = dot(dense_hidden[0], down_keep, FIRST) + dot(dense_hidden[1], down_came, FIRST)
    wide = wide.astype(jnp.bfloat16).reshape(rows, 2 * n_za, width)
    dense_out = lax.psum_scatter(
        jnp.moveaxis(wide, 1, 0), ("za", "zb"), scatter_dimension=0, tiled=False
    )

    odd = dot(jnp.concatenate([gu[1], gu[3]], 0), landed, LAST)
    odd_came = swap(odd, "core", 2, 1)
    even = dot(jnp.concatenate([gu[0], gu[2]], 0), landed, LAST) + odd_came
    far = swap(even[2 * hid :].astype(jnp.bfloat16), "zb", 2, 1)
    gate_up = even[: 2 * hid] + far.astype(jnp.float32)
    hidden = (jax.nn.silu(gate_up[:hid]) * gate_up[hid:]).astype(jnp.bfloat16)

    units = lax.all_gather(hidden, "za", axis=0, tiled=True)
    outgoing = jnp.einsum("kt,qkf->qtf", units, columns, preferred_element_type=jnp.float32)
    outgoing = outgoing.astype(jnp.bfloat16)
    outgoing = outgoing.reshape(4 * experts, slots, width)
    back = lax.all_to_all(outgoing, ("zb", "core", "ep"), split_axis=0, concat_axis=0, tiled=True)

    token = lax.broadcasted_iota(jnp.int32, (rows, experts * slots), 0)
    spread = jnp.where(token == chosen[None, :], pick_weights.reshape(1, -1), 0.0)
    parts = back.reshape(4, experts * slots, width).astype(jnp.float32)
    results = jnp.sum(parts, axis=0).astype(jnp.bfloat16)
    mixture = dot(spread.astype(jnp.bfloat16), results, PLAIN)
    mixed = mixture + jax.nn.sigmoid(branch_gate)[None, :] * dense_out.astype(jnp.float32)
    return mixed.astype(jnp.bfloat16)


def solution(mesh):
    split = Mesh(
        mesh.devices.reshape(mesh.shape["ep"], mesh.shape["tp"] // 4, 2, 2),
        ("ep", "za", "zb", "core"),
    )
    placed = (
        P("ep", TP),
        P("ep", None, None),
        P("ep", None, None),
        P("ep", TP, None),
        P("ep", TP, None),
        P("ep", None, TP),
        P(TP, None),
        P(TP, None),
        P(TP, None),
        P(TP),
    )

    return jax.shard_map(
        per_device, mesh=split, in_specs=placed, out_specs=P("ep", TP), check_vma=False
    )
```

```python
import jax
import jax.numpy as jnp
from jax import lax
from jax.experimental import pallas as pl
from jax.experimental.pallas import tpu as pltpu
from jax.sharding import Mesh
from jax.sharding import PartitionSpec as P


TP = ("za", "zb", "core")
LAST = (((1,), (1,)), ((), ()))
FIRST = (((0,), (0,)), ((), ()))
PLAIN = (((1,), (0,)), ((), ()))
LANES = 128


def expert_kernel(own_ref, gate, up, down, gu_own, gu_far, gu_near, own_out, far_out, near_out):
    own = own_ref[0]
    pairs = (gu_own, gu_near.at[0], gu_far, gu_near.at[1])
    turns = (own_out, near_out.at[0], far_out, near_out.at[1])
    for k in range(4):
        for j in range(own_out.shape[0]):
            tile = j * 4 + (own ^ k)
            row = j * 4 + (own ^ k ^ ((j & 1) ^ own_ref[1]))
            start = pl.multiple_of(tile * LANES, LANES)
            at = slice(j * LANES, (j + 1) * LANES)
            pairs[k][0, :, at] = gate[:, pl.ds(start, LANES)]
            pairs[k][1, :, at] = up[:, pl.ds(start, LANES)]
            turns[k][j] = down[row]


def dense_kernel(own_ref, gate, up, keep, give):
    own = own_ref[0]
    rows = gate.shape[0]
    for k in range(4):
        out = give if k % 2 else keep
        for j in range(out.shape[2] // LANES):
            start = pl.multiple_of((j * 4 + (own ^ k)) * LANES, LANES)
            at = slice(j * LANES, (j + 1) * LANES)
            out[k // 2, :rows, at] = gate[:, pl.ds(start, LANES)]
            out[k // 2, rows:, at] = up[:, pl.ds(start, LANES)]


def down_kernel(own_ref, weight, *outs):
    core = own_ref[0] & 1
    for k, out in enumerate(outs):
        for j in range(out.shape[1] // LANES):
            start = pl.multiple_of((j * 2 + (core ^ k)) * LANES, LANES)
            out[:, j * LANES : (j + 1) * LANES] = weight[:, pl.ds(start, LANES)]


def split_up(kernel, own, outs, *weights):
    return pl.pallas_call(
        kernel,
        out_shape=[jax.ShapeDtypeStruct(shape, jnp.bfloat16) for shape in outs],
        in_specs=[pl.BlockSpec(memory_space=pltpu.SMEM)]
        + [pl.BlockSpec(memory_space=pltpu.VMEM)] * len(weights),
        out_specs=[pl.BlockSpec(memory_space=pltpu.VMEM)] * len(outs),
    )(own.reshape(-1), *weights)


def swap(x, axes, size, k):
    return lax.ppermute(x, axes, [(i, i ^ k) for i in range(size)])


def flat(tiles):
    return jnp.moveaxis(tiles, 0, 1).reshape(tiles.shape[1], -1)


def dot(a, b, dims):
    return lax.dot_general(a, b, dims, preferred_element_type=jnp.float32)


def per_device(
    tokens,
    picks,
    pick_weights,
    gate_weight,
    up_weight,
    down_weight,
    dense_gate,
    dense_up,
    dense_down,
    branch_gate,
):
    quad = lax.axis_index("zb") * 2 + lax.axis_index("core")
    rows, width = tokens.shape
    experts, slots = picks.shape[1:]
    n_za = lax.axis_size("za")
    part = n_za * width
    hid = gate_weight.shape[1]
    dense_hid = dense_gate.shape[0]

    tiles = lax.all_to_all(
        jnp.broadcast_to(tokens, (n_za, rows, width)), "za", split_axis=0, concat_axis=0, tiled=True
    )
    mine = flat(tiles)

    down = down_weight[0].reshape(n_za * 4, hid, width)
    pair, turn = (2, hid, part), (n_za, hid, width)
    gu_own, gu_far, gu_near, turn_own, turn_far, turn_near = split_up(
        expert_kernel,
        jnp.stack([quad, lax.axis_index("za") & 1]),
        [pair, pair, (2, *pair), turn, turn, (2, *turn)],
        gate_weight[0],
        up_weight[0],
        down,
    )
    gu_near = swap(gu_near, "core", 2, 1)
    relay = jnp.stack([gu_far, gu_near[1]])
    gu_far = swap(relay, "zb", 2, 1)
    gu = [gu_own, gu_near[0], gu_far[0], gu_far[1]]
    gu = [x.reshape(2 * hid, part) for x in gu]
    turn_near = swap(turn_near, "core", 2, 1)
    turn_far = swap(jnp.stack([turn_far, turn_near[1]]), "zb", 2, 1)
    turned = jnp.stack([turn_own, turn_near[0], turn_far[0], turn_far[1]])
    turned = turned.reshape(4, n_za * hid, width)
    columns = jnp.stack(
        [lax.dynamic_index_in_dim(turned, quad ^ q, 0, keepdims=False) for q in range(4)]
    )
    dense_keep, dense_give = split_up(
        dense_kernel, quad, [(2, 2 * dense_hid, part)] * 2, dense_gate, dense_up
    )
    dense_came = swap(dense_give, "core", 2, 1)

    down_keep, down_give = split_up(
        down_kernel, quad, [(dense_hid, 2 * part)] * 2, dense_down
    )
    down_came = swap(down_give, "core", 2, 1)

    chosen = picks.reshape(-1)
    pick_matrix = (
        lax.broadcasted_iota(jnp.int32, (experts * slots, rows), 1) == chosen[:, None]
    ).astype(jnp.bfloat16)
    picked = dot(pick_matrix, mine, PLAIN).astype(jnp.bfloat16)
    picked = picked.reshape(experts, slots, part)
    landed = lax.all_to_all(picked, "ep", split_axis=0, concat_axis=0, tiled=True)
    landed = landed.reshape(-1, part)

    tiles_far = swap(tiles, "zb", 2, 1)
    firsts = [dot(w[0], mine, LAST) for w in (dense_keep, dense_came)]
    firsts = lax.optimization_barrier(firsts)
    theirs = flat(tiles_far)
    own_part, pair_part = (
        first + dot(w[1], theirs, LAST) for first, w in zip(firsts, (dense_keep, dense_came))
    )
    came_part = swap(jnp.stack([pair_part, own_part]), "core", 2, 1)
    dense_hidden = []
    for gu_sum in (own_part + came_part[0], pair_part + came_part[1]):
        value = jax.nn.silu(gu_sum[:dense_hid]) * gu_sum[dense_hid:]
        dense_hidden.append(value.astype(jnp.bfloat16))
    wide = dot(dense_hidden[0], down_keep, FIRST) + dot(dense_hidden[1], down_came, FIRST)
    wide = wide.astype(jnp.bfloat16).reshape(rows, 2 * n_za, width)
    dense_out = lax.psum_scatter(
        jnp.moveaxis(wide, 1, 0), ("za", "zb"), scatter_dimension=0, tiled=False
    )

    odd = dot(jnp.concatenate([gu[1], gu[3]], 0), landed, LAST)
    odd_came = swap(odd, "core", 2, 1)
    even = dot(jnp.concatenate([gu[0], gu[2]], 0), landed, LAST) + odd_came
    far = swap(even[2 * hid :].astype(jnp.bfloat16), "zb", 2, 1)
    gate_up = even[: 2 * hid] + far.astype(jnp.float32)
    hidden = (jax.nn.silu(gate_up[:hid]) * gate_up[hid:]).astype(jnp.bfloat16)

    rings = [[chip * 2 + ((chip ^ k) & 1) for chip in range(n_za)] for k in range(2)]
    units = lax.all_gather(
        hidden, ("za", "core"), axis=0, tiled=True, axis_index_groups=rings
    )
    outgoing = jnp.einsum("kt,qkf->qtf", units, columns, preferred_element_type=jnp.float32)
    outgoing = outgoing.astype(jnp.bfloat16)
    outgoing = outgoing.reshape(4 * experts, slots, width)
    back = lax.all_to_all(outgoing, ("zb", "core", "ep"), split_axis=0, concat_axis=0, tiled=True)

    token = lax.broadcasted_iota(jnp.int32, (rows, experts * slots), 0)
    spread = jnp.where(token == chosen[None, :], pick_weights.reshape(1, -1), 0.0)
    parts = back.reshape(4, experts * slots, width).astype(jnp.float32)
    results = jnp.sum(parts, axis=0).astype(jnp.bfloat16)
    mixture = dot(spread.astype(jnp.bfloat16), results, PLAIN)
    mixed = mixture + jax.nn.sigmoid(branch_gate)[None, :] * dense_out.astype(jnp.float32)
    return mixed.astype(jnp.bfloat16)


def solution(mesh):
    split = Mesh(
        mesh.devices.reshape(mesh.shape["ep"], mesh.shape["tp"] // 4, 2, 2),
        ("ep", "za", "zb", "core"),
    )
    placed = (
        P("ep", TP),
        P("ep", None, None),
        P("ep", None, None),
        P("ep", TP, None),
        P("ep", TP, None),
        P("ep", None, TP),
        P(TP, None),
        P(TP, None),
        P(TP, None),
        P(TP),
    )

    return jax.shard_map(
        per_device, mesh=split, in_specs=placed, out_specs=P("ep", TP), check_vma=False
    )
```

```python
import jax
import jax.numpy as jnp
from jax import lax
from jax.experimental import pallas as pl
from jax.experimental.pallas import tpu as pltpu
from jax.sharding import Mesh
from jax.sharding import PartitionSpec as P


TP = ("za", "zb", "core")
LAST = (((1,), (1,)), ((), ()))
FIRST = (((0,), (0,)), ((), ()))
PLAIN = (((1,), (0,)), ((), ()))
LANES = 128


def expert_kernel(own_ref, gate, up, down, gu_own, gu_far, gu_near, own_out, far_out, near_out):
    own = own_ref[0]
    pairs = (gu_own, gu_near.at[0], gu_far, gu_near.at[1])
    turns = (own_out, near_out.at[0], far_out, near_out.at[1])
    for k in range(4):
        for j in range(own_out.shape[0]):
            tile = j * 4 + (own ^ k)
            row = j * 4 + (own ^ k ^ ((j & 1) ^ own_ref[1]))
            start = pl.multiple_of(tile * LANES, LANES)
            at = slice(j * LANES, (j + 1) * LANES)
            pairs[k][0, :, at] = gate[:, pl.ds(start, LANES)]
            pairs[k][1, :, at] = up[:, pl.ds(start, LANES)]
            turns[k][j] = down[row]


def dense_kernel(own_ref, gate, up, keep, give):
    own = own_ref[0]
    rows = gate.shape[0]
    for k in range(4):
        out = give if k % 2 else keep
        for j in range(out.shape[2] // LANES):
            start = pl.multiple_of((j * 4 + (own ^ k)) * LANES, LANES)
            at = slice(j * LANES, (j + 1) * LANES)
            out[k // 2, :rows, at] = gate[:, pl.ds(start, LANES)]
            out[k // 2, rows:, at] = up[:, pl.ds(start, LANES)]


def down_kernel(own_ref, weight, *outs):
    core = own_ref[0] & 1
    for k, out in enumerate(outs):
        for j in range(out.shape[1] // LANES):
            start = pl.multiple_of((j * 2 + (core ^ k)) * LANES, LANES)
            out[:, j * LANES : (j + 1) * LANES] = weight[:, pl.ds(start, LANES)]


def split_up(kernel, own, outs, *weights):
    return pl.pallas_call(
        kernel,
        out_shape=[jax.ShapeDtypeStruct(shape, jnp.bfloat16) for shape in outs],
        in_specs=[pl.BlockSpec(memory_space=pltpu.SMEM)]
        + [pl.BlockSpec(memory_space=pltpu.VMEM)] * len(weights),
        out_specs=[pl.BlockSpec(memory_space=pltpu.VMEM)] * len(outs),
    )(own.reshape(-1), *weights)


def swap(x, axes, size, k):
    return lax.ppermute(x, axes, [(i, i ^ k) for i in range(size)])


def flat(tiles):
    return jnp.moveaxis(tiles, 0, 1).reshape(tiles.shape[1], -1)


def dot(a, b, dims):
    return lax.dot_general(a, b, dims, preferred_element_type=jnp.float32)


def per_device(
    tokens,
    picks,
    pick_weights,
    gate_weight,
    up_weight,
    down_weight,
    dense_gate,
    dense_up,
    dense_down,
    branch_gate,
):
    quad = lax.axis_index("zb") * 2 + lax.axis_index("core")
    rows, width = tokens.shape
    experts, slots = picks.shape[1:]
    n_za = lax.axis_size("za")
    part = n_za * width
    hid = gate_weight.shape[1]
    dense_hid = dense_gate.shape[0]

    tiles = lax.all_to_all(
        jnp.broadcast_to(tokens, (n_za, rows, width)), "za", split_axis=0, concat_axis=0, tiled=True
    )
    mine = flat(tiles)

    down = down_weight[0].reshape(n_za * 4, hid, width)
    pair, turn = (2, hid, part), (n_za, hid, width)
    gu_own, gu_far, gu_near, turn_own, turn_far, turn_near = split_up(
        expert_kernel,
        jnp.stack([quad, lax.axis_index("za") & 1]),
        [pair, pair, (2, *pair), turn, turn, (2, *turn)],
        gate_weight[0],
        up_weight[0],
        down,
    )
    gu_near = swap(gu_near, "core", 2, 1)
    relay = jnp.stack([gu_far, gu_near[1]])
    gu_far = swap(relay, "zb", 2, 1)
    gu = [gu_own, gu_near[0], gu_far[0], gu_far[1]]
    gu = [x.reshape(2 * hid, part) for x in gu]
    turn_near = swap(turn_near, "core", 2, 1)
    turn_far = swap(jnp.stack([turn_far, turn_near[1]]), "zb", 2, 1)
    turned = jnp.stack([turn_own, turn_near[0], turn_far[0], turn_far[1]])
    turned = turned.reshape(4, n_za * hid, width)
    columns = jnp.stack(
        [lax.dynamic_index_in_dim(turned, quad ^ q, 0, keepdims=False) for q in range(4)]
    )
    dense_keep, dense_give = split_up(
        dense_kernel, quad, [(2, 2 * dense_hid, part)] * 2, dense_gate, dense_up
    )
    dense_came = swap(dense_give, "core", 2, 1)

    down_keep, down_give = split_up(
        down_kernel, quad, [(dense_hid, 2 * part)] * 2, dense_down
    )
    down_came = swap(down_give, "core", 2, 1)

    chosen = picks.reshape(-1)
    pick_matrix = (
        lax.broadcasted_iota(jnp.int32, (experts * slots, rows), 1) == chosen[:, None]
    ).astype(jnp.bfloat16)
    picked = dot(pick_matrix, mine, PLAIN).astype(jnp.bfloat16)
    picked = picked.reshape(experts, slots, part)
    landed = lax.all_to_all(picked, "ep", split_axis=0, concat_axis=0, tiled=True)
    landed = landed.reshape(-1, part)

    tiles_far = swap(tiles, "zb", 2, 1)
    firsts = [dot(w[0], mine, LAST) for w in (dense_keep, dense_came)]
    firsts = lax.optimization_barrier(firsts)
    theirs = flat(tiles_far)
    own_part, pair_part = (
        first + dot(w[1], theirs, LAST) for first, w in zip(firsts, (dense_keep, dense_came))
    )
    outgoing_part = jnp.stack([pair_part, own_part]).astype(jnp.bfloat16)
    came_part = swap(outgoing_part, "core", 2, 1).astype(jnp.float32)
    dense_hidden = []
    for gu_sum in (own_part + came_part[0], pair_part + came_part[1]):
        value = jax.nn.silu(gu_sum[:dense_hid]) * gu_sum[dense_hid:]
        dense_hidden.append(value.astype(jnp.bfloat16))
    wide = dot(dense_hidden[0], down_keep, FIRST) + dot(dense_hidden[1], down_came, FIRST)
    wide = wide.astype(jnp.bfloat16).reshape(rows, 2 * n_za, width)
    dense_out = lax.psum_scatter(
        jnp.moveaxis(wide, 1, 0), ("za", "zb"), scatter_dimension=0, tiled=False
    )

    odd = dot(jnp.concatenate([gu[1], gu[3]], 0), landed, LAST)
    odd_came = swap(odd.astype(jnp.bfloat16), "core", 2, 1).astype(jnp.float32)
    even = dot(jnp.concatenate([gu[0], gu[2]], 0), landed, LAST) + odd_came
    far = swap(even[2 * hid :].astype(jnp.bfloat16), "zb", 2, 1)
    gate_up = even[: 2 * hid] + far.astype(jnp.float32)
    hidden = (jax.nn.silu(gate_up[:hid]) * gate_up[hid:]).astype(jnp.bfloat16)

    rings = [[chip * 2 + ((chip ^ k) & 1) for chip in range(n_za)] for k in range(2)]
    units = lax.all_gather(
        hidden, ("za", "core"), axis=0, tiled=True, axis_index_groups=rings
    )
    outgoing = jnp.einsum("kt,qkf->qtf", units, columns, preferred_element_type=jnp.float32)
    outgoing = outgoing.astype(jnp.bfloat16)
    outgoing = outgoing.reshape(4 * experts, slots, width)
    back = lax.all_to_all(outgoing, ("zb", "core", "ep"), split_axis=0, concat_axis=0, tiled=True)

    gated = jax.nn.sigmoid(branch_gate)[None, :] * dense_out.astype(jnp.float32)
    gated = lax.optimization_barrier(gated)
    token = lax.broadcasted_iota(jnp.int32, (rows, experts * slots), 0)
    spread = jnp.where(token == chosen[None, :], pick_weights.reshape(1, -1), 0.0)
    parts = back.reshape(4, experts * slots, width).astype(jnp.float32)
    results = jnp.sum(parts, axis=0).astype(jnp.bfloat16)
    spread = lax.optimization_barrier(spread.astype(jnp.bfloat16))
    mixture = dot(spread, results, PLAIN)
    mixed = mixture + gated
    return mixed.astype(jnp.bfloat16)


def solution(mesh):
    split = Mesh(
        mesh.devices.reshape(mesh.shape["ep"], mesh.shape["tp"] // 4, 2, 2),
        ("ep", "za", "zb", "core"),
    )
    placed = (
        P("ep", TP),
        P("ep", None, None),
        P("ep", None, None),
        P("ep", TP, None),
        P("ep", TP, None),
        P("ep", None, TP),
        P(TP, None),
        P(TP, None),
        P(TP, None),
        P(TP),
    )

    return jax.shard_map(
        per_device, mesh=split, in_specs=placed, out_specs=P("ep", TP), check_vma=False
    )
```
